32 devices in a mesh: grp: 2 (over x), ep: 16 (over z, y, core).
Axes of the slice: x: 2, y: 2, z: 4, core: 2. Of those that a mesh axis runs over, the one named last changes fastest.
Arguments:
- residual: bfloat16 [16, 4096], P('grp', 'ep'), parts along dimension 0, may hold values from -6 to 6
- head_states: float32 [64, 512, 1024], P(('grp', 'ep')), parts along dimension 0, may hold values from -6 to 6
- first_gain: bfloat16 [4096], replicated, may hold values from 0.099609375 to 1.8984375
- w_query: bfloat16 [4096, 2048], P(None, 'ep'), may hold values from -0.09375 to 0.09375
- w_key: bfloat16 [4096, 2048], P(None, 'ep'), may hold values from -0.09375 to 0.09375
- w_value: bfloat16 [4096, 4096], P(None, 'ep'), may hold values from -0.09375 to 0.09375
- w_gate: bfloat16 [4096, 4096], P(None, 'ep'), may hold values from -0.09375 to 0.09375
- w_low: bfloat16 [4096, 16], replicated, may hold values from -0.09375 to 0.09375
- w_decay: bfloat16 [16, 2048], replicated, may hold values from -15 to 15
- decay_bias: float32 [2048], replicated, may hold values from -40 to 4
- head_gain: bfloat16 [1024], replicated, may hold values from 0.099609375 to 1.8984375
- w_output: bfloat16 [4096, 4096], P(None, 'ep'), may hold values from -0.09375 to 0.09375
- second_gain: bfloat16 [4096], replicated, may hold values from 0.099609375 to 1.8984375
- routes: int32 [16, 2], P('grp'), parts along dimension 0, may hold values from 0 to 15, as said below
- group_logits: float32 [16, 4], P('grp'), parts along dimension 0, may hold values from -12 to 12
- expert_logits: float32 [16, 2], P('grp'), parts along dimension 0, may hold values from -9 to 9
- expert_gate: bfloat16 [16, 4096, 512], P('ep'), may hold values from -0.09375 to 0.09375
- expert_up: bfloat16 [16, 4096, 512], P('ep'), may hold values from -0.09375 to 0.09375
- expert_down: bfloat16 [16, 512, 4096], P('ep'), may hold values from -0.25 to 0.25
Outputs:
- layer_out: bfloat16 [16, 4096], P('grp', 'ep'), parts along dimension 0
- new_states: float32 [64, 512, 1024], P(('grp', 'ep')), parts along dimension 0
The draws below stay inside these ranges and needn't reach their ends.
There are 2 independent parts, one for each index of `grp`. The reference program is written for one: setup_inputs(seed, part) draws one part's arguments, and reference() takes and returns one part's arrays. A program takes and returns all parts, laid end to end along the dimension named above; an argument that names none is the same for every part. Nothing has to cross between parts.
Inputs may be any that keep to these rules, and one draw needn't show every extreme that they name: `routes`: each row names 2 different experts of one group (numbers g * 4 to g * 4 + 3). No expert is named by more than 2 rows, and in every draw all experts of one group are named by exactly 2 rows.
All inputs are finite; a program needn't handle non-finite values.
Results may differ from the reference program's by a relative error of at most 0.014.
Values may be sent and summed in bfloat16 or wider, within the bound.
No kernel may reach another device: no remote copies, remote signals or barrier semaphores. Data moves between devices by JAX's collectives and lax.ppermute only.
A program may use at most 128 MiB of HBM per device.

```python
import jax
import jax.numpy as jnp
from jax import lax

D = 4096
HEADS = 4
DK = 512
DV = 1024
RANK = 16
FF = 512
GROUPS = 4
TOP = 2
SEQS = 8
PAIRS = 32
EXPERTS = 16
EPG = 4
CAP = 2


def draw_routes(key, part):
    order_key, full_key, other_key, perm_key = jax.random.split(jax.random.fold_in(key, 17), 4)
    full_count = EPG * CAP // TOP
    order = jax.random.permutation(order_key, SEQS)
    full_group = jax.random.randint(full_key, (), 0, GROUPS, dtype=jnp.int32)
    others = jax.random.randint(other_key, (SEQS,), 0, GROUPS - 1, dtype=jnp.int32)
    others = others + (others >= full_group).astype(jnp.int32)
    position = jnp.arange(SEQS, dtype=jnp.int32)
    by_position = jnp.where(position < full_count, full_group, others)
    group = jnp.zeros((SEQS,), jnp.int32).at[order].set(by_position)
    member = (group[:, None] == jnp.arange(GROUPS, dtype=jnp.int32)[None, :]).astype(jnp.int32)
    before = jnp.cumsum(member, axis=0) - member
    rank = jnp.sum(before * member, axis=1)
    tables = jax.vmap(lambda one: jax.random.permutation(one, EPG))(jax.random.split(perm_key, GROUPS)).astype(jnp.int32)
    slots = TOP * rank[:, None] + jnp.arange(TOP, dtype=jnp.int32)[None, :]
    local = slots % EPG
    chosen = tables[group[:, None], local]
    return (group[:, None] * EPG + chosen).astype(jnp.int32)


def steps_of(own_key, dims, pieces, low, largest):
    factor_of, own = 1.0, jax.random.fold_in(own_key, 6)
    for dim, parts in pieces:
        steps = jnp.exp(jax.random.uniform(jax.random.fold_in(own, dim), (parts,), jnp.float32, low / len(pieces), largest / len(pieces)))
        factor_of = factor_of * jnp.repeat(steps, dims[dim] // parts).reshape([-1 if axis == dim else 1 for axis in range(len(dims))])
    return factor_of


def gaussian(rng, extent, scale, bound, cuts=(), held_as=jnp.bfloat16):
    level = steps_of(rng, extent, cuts, -0.22, 0.18) if cuts else 1.0
    array = jax.random.normal(rng, extent, jnp.float32) * scale * level
    return jnp.minimum(jnp.maximum(array, -bound), bound).astype(held_as)


def setup_inputs(seed: int = 0, part: int = 0) -> dict:
    arg_keys = jax.random.split(jax.random.key(seed), 20)
    part_splits = jax.random.split(jax.random.fold_in(arg_keys[19], part), 20)
    return {
        "residual": gaussian(part_splits[0], (SEQS, D), 1.0, 6.0, ((1, 16),)),
        "head_states": gaussian(part_splits[1], (PAIRS, DK, DV), 1.0, 6.0, ((0, 16),), jnp.float32),
        "first_gain": jnp.clip(1.0 + 0.18 * jax.random.normal(arg_keys[2], (D,), jnp.float32), 0.099609375, 1.8984375).astype(jnp.bfloat16),
        "w_query": gaussian(arg_keys[3], (D, HEADS * DK), D ** -0.5, 0.09375, ((1, 16),)),
        "w_key": gaussian(arg_keys[4], (D, HEADS * DK), D ** -0.5, 0.09375, ((1, 16),)),
        "w_value": gaussian(arg_keys[5], (D, HEADS * DV), D ** -0.5, 0.09375, ((1, 16),)),
        "w_gate": gaussian(arg_keys[6], (D, HEADS * DV), D ** -0.5, 0.09375, ((1, 16),)),
        "w_low": gaussian(arg_keys[7], (D, RANK), D ** -0.5, 0.09375),
        "w_decay": gaussian(arg_keys[8], (RANK, HEADS * DK), 3.0, 15.0),
        "decay_bias": jnp.clip(jax.random.uniform(arg_keys[9], (HEADS * DK,), jnp.float32, -40.0, 4.0), -40.0, 4.0),
        "head_gain": jnp.clip(1.0 + 0.18 * jax.random.normal(arg_keys[10], (DV,), jnp.float32), 0.099609375, 1.8984375).astype(jnp.bfloat16),
        "w_output": gaussian(arg_keys[11], (HEADS * DV, D), (HEADS * DV) ** -0.5, 0.09375, ((1, 16),)),
        "second_gain": jnp.clip(1.0 + 0.18 * jax.random.normal(arg_keys[12], (D,), jnp.float32), 0.099609375, 1.8984375).astype(jnp.bfloat16),
        "routes": draw_routes(jax.random.fold_in(jax.random.fold_in(arg_keys[19], part), 71), part),
        "group_logits": gaussian(part_splits[14], (SEQS, GROUPS), 2.0, 12.0, (), jnp.float32),
        "expert_logits": gaussian(part_splits[15], (SEQS, TOP), 1.5, 9.0, (), jnp.float32),
        "expert_gate": gaussian(arg_keys[16], (EXPERTS, D, FF), D ** -0.5, 0.09375, ((0, 16),)),
        "expert_up": gaussian(arg_keys[17], (EXPERTS, D, FF), D ** -0.5, 0.09375, ((0, 16),)),
        "expert_down": gaussian(arg_keys[18], (EXPERTS, FF, D), FF ** -0.5, 0.25, ((0, 16),)),
    }


norm_eps = 1e-06
decay_tau = 16.0

def rms_scale(values, gain):
    floats = values.astype(jnp.float32)
    return floats * lax.rsqrt(lax.optimization_barrier(jnp.mean(floats * floats, axis=-1, keepdims=True)) + norm_eps) * gain.astype(jnp.float32)

def route_weights(routes, group_logits, expert_logits, per_group):
    group_exp = jnp.exp(group_logits)
    group_prob = group_exp / lax.optimization_barrier(jnp.sum(group_exp, axis=1, keepdims=True))
    chosen = routes[:, 0] // per_group
    groups_row = jnp.arange(group_logits.shape[1], dtype=jnp.int32)
    picked = lax.optimization_barrier(jnp.sum(group_prob * (chosen[:, None] == groups_row[None, :]).astype(jnp.float32), axis=1))
    expert_exp = jnp.exp(expert_logits)
    return expert_exp / lax.optimization_barrier(jnp.sum(expert_exp, axis=1, keepdims=True)) * picked[:, None]

def reference(residual, head_states, first_gain, w_query, w_key, w_value, w_gate, w_low, w_decay, decay_bias, head_gain, w_output, second_gain, routes, group_logits, expert_logits, expert_gate, expert_up, expert_down):
    normed = rms_scale(residual, first_gain).astype(jnp.bfloat16)
    query = jnp.dot(normed, w_query, preferred_element_type=jnp.float32).astype(jnp.bfloat16).reshape(PAIRS, DK)
    key = jnp.dot(normed, w_key, preferred_element_type=jnp.float32).astype(jnp.bfloat16).reshape(PAIRS, DK)
    value = jnp.dot(normed, w_value, preferred_element_type=jnp.float32).astype(jnp.bfloat16).reshape(PAIRS, DV)
    gate = jnp.dot(normed, w_gate, preferred_element_type=jnp.float32).astype(jnp.bfloat16).reshape(PAIRS, DV)
    low = jnp.dot(normed, w_low, preferred_element_type=jnp.float32)
    decay_pre = jnp.dot(low, w_decay.astype(jnp.float32), precision=lax.Precision.HIGHEST) + decay_bias
    log_decay = jax.nn.log_sigmoid(decay_pre.reshape(PAIRS, DK)) / decay_tau
    new_states = head_states * jnp.exp(log_decay)[:, :, None] + key.astype(jnp.float32)[:, :, None] * value.astype(jnp.float32)[:, None, :]
    read = jnp.einsum('pk,pkv->pv', query.astype(jnp.float32) * DK ** (-0.5), new_states, precision=lax.Precision.HIGHEST)
    mixed = (rms_scale(read, head_gain) * jax.nn.silu(gate.astype(jnp.float32))).astype(jnp.bfloat16)
    branch = jnp.dot(mixed.reshape(SEQS, HEADS * DV), w_output, preferred_element_type=jnp.float32).astype(jnp.bfloat16)
    stream = (residual.astype(jnp.float32) + branch.astype(jnp.float32)).astype(jnp.bfloat16)
    expert_in = rms_scale(stream, second_gain).astype(jnp.bfloat16)
    weights = route_weights(routes, group_logits, expert_logits, EPG)
    every = jnp.arange(EXPERTS, dtype=jnp.int32)
    combine = lax.optimization_barrier(jnp.sum(weights[:, :, None] * (routes[:, :, None] == every[None, None, :]).astype(jnp.float32), axis=1))

    def one_expert(total, inputs):
        gate_w, up_w, down_w, share = inputs
        gate_part = jnp.dot(expert_in, gate_w, preferred_element_type=jnp.float32)
        up_part = jnp.dot(expert_in, up_w, preferred_element_type=jnp.float32)
        active = (jax.nn.silu(gate_part) * up_part * share[:, None]).astype(jnp.bfloat16)
        contribution = jnp.dot(active, down_w, preferred_element_type=jnp.float32).astype(jnp.bfloat16)
        return (total + contribution.astype(jnp.float32), None)
    start = jnp.zeros((SEQS, D), jnp.float32)
    summed, _ = lax.scan(one_expert, start, (expert_gate, expert_up, expert_down, combine.T))
    layer_out = (stream.astype(jnp.float32) + summed).astype(jnp.bfloat16)
    return (layer_out, new_states)
```

```python
import functools

import jax
import jax.numpy as jnp
from jax import lax
from jax.experimental import pallas as pl
from jax.experimental.pallas import tpu as pltpu
from jax.sharding import PartitionSpec as P

HEADS = 4
GROUPS = 4
LANES = 128

norm_eps = 1e-06
decay_tau = 16.0
f32 = jnp.float32
bf16 = jnp.bfloat16

ANY = pl.BlockSpec(memory_space=pl.ANY)
VMEM = pl.BlockSpec(memory_space=pltpu.VMEM)
SMEM = pl.BlockSpec(memory_space=pltpu.SMEM)


def route_weights(routes, group_logits, expert_logits, per_group):
    group_exp = jnp.exp(group_logits)
    group_prob = group_exp / jnp.sum(group_exp, axis=1, keepdims=True)
    chosen = routes[:, 0] // per_group
    groups_row = jnp.arange(group_logits.shape[1], dtype=jnp.int32)
    picked = jnp.sum(
        group_prob * (chosen[:, None] == groups_row[None, :]).astype(f32), axis=1
    )
    expert_exp = jnp.exp(expert_logits)
    return expert_exp / jnp.sum(expert_exp, axis=1, keepdims=True) * picked[:, None]


def start_chunks(pairs, sems, chunks):
    started = []
    for c in range(chunks):
        row = []
        for n, (src, dst) in enumerate(pairs):
            size = src.shape[0] // chunks
            rows = pl.ds(c * size, size)
            copy = pltpu.make_async_copy(src.at[rows], dst.at[rows], sems.at[n, c])
            copy.start()
            row.append(copy)
        started.append(row)
    return started


def normed_rows(blocks_ref, gain_ref):
    count, _, own = blocks_ref.shape
    total = None
    for j in range(count):
        x = blocks_ref[j].astype(f32)
        total = x * x if total is None else total + x * x
    mean = jnp.sum(total, axis=1, keepdims=True) / (count * own)
    scale = lax.rsqrt(mean + norm_eps)
    out = []
    for j in range(count):
        gain = gain_ref[:, j * own : (j + 1) * own].astype(f32)
        out.append((blocks_ref[j].astype(f32) * scale * gain).astype(bf16))
    return jnp.concatenate(out, axis=1)


def project_kernel(
    chunks, blocks_ref, gain_ref, low_w_ref, wq, wk, wv, wg, send_ref, low_ref, bq, bk, bv, bg, sems
):
    started = start_chunks(((wq, bq), (wk, bk), (wv, bv), (wg, bg)), sems, chunks)
    normed = normed_rows(blocks_ref, gain_ref)
    low_ref[...] = lax.dot_general(
        low_w_ref[...], normed, (((1,), (1,)), ((), ())), preferred_element_type=f32
    )
    size = bq.shape[0] // chunks
    sums = [None] * 4
    for c in range(chunks):
        part = normed[:, c * size : (c + 1) * size]
        for n, buf in enumerate((bq, bk, bv, bg)):
            started[c][n].wait()
            one = jnp.dot(part, buf[c * size : (c + 1) * size, :], preferred_element_type=f32)
            sums[n] = one if sums[n] is None else sums[n] + one
    projected = jnp.concatenate(sums, axis=1).astype(bf16).astype(f32)
    rows = projected.shape[1] // LANES
    tokens = projected.shape[0]
    times = send_ref.shape[0] // tokens
    pad = jnp.zeros((send_ref.shape[1] - rows, LANES), f32)
    for s in range(tokens):
        tile = jnp.concatenate(
            [projected[s : s + 1, r * LANES : (r + 1) * LANES] for r in range(rows)] + [pad], axis=0
        )
        for t in range(times):
            send_ref[s * times + t] = tile


def decay_kernel(seq_ref, low_ref, w_ref, bias_ref, out_ref):
    lane = lax.broadcasted_iota(jnp.int32, low_ref.shape, 1)
    low = jnp.sum(jnp.where(lane == seq_ref[0], low_ref[...], 0.0), axis=1, keepdims=True)
    pre = jnp.sum(w_ref[...].astype(f32) * low, axis=0, keepdims=True) + bias_ref[...]
    log_decay = (jnp.minimum(pre, 0.0) - jnp.log1p(jnp.exp(-jnp.abs(pre)))) / decay_tau
    decay = jnp.exp(log_decay)
    wide = out_ref.shape[2]
    for r in range(out_ref.shape[0]):
        out_ref[r] = decay[:, r * wide : (r + 1) * wide]


def tile_columns(tile, decay, qw):
    if qw < LANES:
        decay = jnp.concatenate([decay, jnp.zeros((1, LANES - qw), f32)], axis=1)
    row = lax.broadcasted_iota(jnp.int32, tile.shape, 0)
    turned = jnp.where(row == tile.shape[0] - 1, decay, tile).T
    last = tile.shape[0] - 1

    def column(at):
        return turned[at % LANES : at % LANES + qw, at // LANES : at // LANES + 1]

    return column(0), column(qw), turned[:qw, last : last + 1]


def wide_row(tiles, at, width):
    pieces = []
    for tile in tiles:
        for lane in range(at, at + width, LANES):
            pieces.append(tile[lane // LANES : lane // LANES + 1, :])
    return jnp.concatenate(pieces, axis=1)


def read_kernel(qw, vw, tiles_ref, decay_ref, gain_ref, states, send_ref, buf, sems):
    pairs, dk, dv = states.shape
    sources = dk // qw
    copies = []
    for p in range(pairs):
        for i in range(sources):
            rows = pl.ds(i * qw, qw)
            copy = pltpu.make_async_copy(
                states.at[p, rows], buf.at[p, rows], sems.at[p, i]
            )
            copy.start()
            copies.append(copy)
    lines = []
    for p in range(pairs):
        tiles = [tiles_ref[p * sources + i] for i in range(sources)]
        value = wide_row(tiles, 2 * qw, vw)
        gate = wide_row(tiles, 2 * qw + vw, vw)
        total = jnp.zeros((8, dv), f32)
        both = jnp.zeros((), f32)
        for i in range(sources):
            query, key, decay = tile_columns(tiles[i], decay_ref[p * sources + i], qw)
            both = both + jnp.sum(query * key)
            factor = query * decay
            copies[p * sources + i].wait()
            for g in range(qw // 8):
                at = i * qw + g * 8
                total = total + buf[p, at : at + 8, :] * factor[g * 8 : g * 8 + 8]
        read = (jnp.sum(total, axis=0, keepdims=True) + both * value) * dk ** (-0.5)
        mean = jnp.sum(read * read, axis=1, keepdims=True) / dv
        line = read * lax.rsqrt(mean + norm_eps) * gain_ref[...].astype(f32)
        line = line * (gate * (1.0 / (1.0 + jnp.exp(-gate))))
        lines += [line[:, c * LANES : (c + 1) * LANES] for c in range(dv // LANES)]
    mixed = jnp.concatenate(lines, axis=0).astype(bf16)
    for d in range(send_ref.shape[0]):
        send_ref[d] = mixed


def update_kernel(qw, vw, sources, tiles_ref, decay_ref, state_ref, out_ref):
    p, i = pl.program_id(0), pl.program_id(1)
    tiles = [tiles_ref[p * sources + n] for n in range(sources)]
    value = wide_row(tiles, 2 * qw, vw)
    _, key, decay = tile_columns(tiles_ref[p * sources + i], decay_ref[p * sources + i], qw)
    out_ref[0] = state_ref[0] * decay + key * value


def branch_kernel(chunks, got_ref, res_ref, w, stream_ref, send_ref, buf, sems):
    started = start_chunks(((w, buf),), sems, chunks)
    tokens = res_ref.shape[0]
    parts = got_ref[...].astype(f32).reshape(tokens, -1, LANES)
    parts = jnp.swapaxes(parts, 0, 1)
    size = buf.shape[0] // chunks
    total = None
    for c in range(chunks):
        each = size // LANES
        part = jnp.concatenate([parts[c * each + m] for m in range(each)], axis=1).astype(bf16)
        started[c][0].wait()
        one = jnp.dot(part, buf[c * size : (c + 1) * size, :], preferred_element_type=f32)
        total = one if total is None else total + one
    stream = (res_ref[...].astype(f32) + total.astype(bf16).astype(f32)).astype(bf16)
    stream_ref[...] = stream
    for d in range(send_ref.shape[0]):
        send_ref[d] = stream


def expert_kernel(
    chunks, blocks_ref, gain_ref, share_ref, wg, wu, wd, send_ref, bg, bu, bd, sems, dsems
):
    started = start_chunks(((wg.at[0], bg), (wu.at[0], bu)), sems, chunks)
    own = send_ref.shape[2]
    pieces = 4
    wide = bd.shape[1] // pieces
    downs = []
    for c in range(pieces):
        columns = pl.ds(c * wide, wide)
        copy = pltpu.make_async_copy(wd.at[0, :, columns], bd.at[:, columns], dsems.at[c])
        copy.start()
        downs.append(copy)
    normed = normed_rows(blocks_ref, gain_ref)
    size = bg.shape[0] // chunks
    gate = up = None
    for c in range(chunks):
        part = normed[:, c * size : (c + 1) * size]
        started[c][0].wait()
        one = jnp.dot(part, bg[c * size : (c + 1) * size, :], preferred_element_type=f32)
        gate = one if gate is None else gate + one
        started[c][1].wait()
        one = jnp.dot(part, bu[c * size : (c + 1) * size, :], preferred_element_type=f32)
        up = one if up is None else up + one
    active = gate * (1.0 / (1.0 + jnp.exp(-gate))) * up * share_ref[...]
    active = active.astype(bf16)
    for c in range(pieces):
        downs[c].wait()
        one = jnp.dot(active, bd[:, c * wide : (c + 1) * wide], preferred_element_type=f32)
        one = one.astype(bf16)
        for n in range(wide // own):
            send_ref[c * (wide // own) + n] = one[:, n * own : (n + 1) * own]


def cost(nbytes):
    return pl.CostEstimate(flops=nbytes, bytes_accessed=nbytes, transcendentals=0)


def exchange(blocks):
    return lax.all_to_all(blocks, "ep", split_axis=0, concat_axis=0, tiled=True)


def per_device(
    residual,
    head_states,
    first_gain,
    w_query,
    w_key,
    w_value,
    w_gate,
    w_low,
    w_decay,
    decay_bias,
    head_gain,
    w_output,
    second_gain,
    routes,
    group_logits,
    expert_logits,
    expert_gate,
    expert_up,
    expert_down,
):
    devices = lax.axis_size("ep")
    me = lax.axis_index("ep")
    tokens, own = residual.shape
    width = own * devices
    pairs, dk, dv = head_states.shape
    qw, vw = w_query.shape[1], w_value.shape[1]
    sources = devices // HEADS
    rank = w_low.shape[1]
    ff = expert_gate.shape[2]
    tile = jax.ShapeDtypeStruct

    arrived = exchange(jnp.broadcast_to(residual[None], (devices, tokens, own)))

    first_pair = me * pairs
    first_head = lax.rem(first_pair, HEADS)
    decay_w = lax.dynamic_slice_in_dim(w_decay, first_head * dk, pairs * dk, 1)
    decay_b = lax.dynamic_slice_in_dim(decay_bias, first_head * dk, pairs * dk, 0)
    weights = route_weights(routes, group_logits, expert_logits, devices // GROUPS)
    share = jnp.sum(weights * (routes == me).astype(f32), axis=1)[:, None]

    chunks = 4
    send, low = pl.pallas_call(
        functools.partial(project_kernel, chunks),
        out_shape=(tile((devices, 8, LANES), f32), tile((rank, tokens), f32)),
        in_specs=[VMEM] * 3 + [ANY] * 4,
        out_specs=(VMEM, VMEM),
        scratch_shapes=[
            pltpu.VMEM((width, qw), bf16),
            pltpu.VMEM((width, qw), bf16),
            pltpu.VMEM((width, vw), bf16),
            pltpu.VMEM((width, vw), bf16),
            pltpu.SemaphoreType.DMA((4, chunks)),
        ],
        cost_estimate=cost(width * (qw + vw) * 4),
        name="project",
    )(arrived, first_gain[None, :], w_low.T, w_query, w_key, w_value, w_gate)
    got = exchange(send)

    decay = pl.pallas_call(
        decay_kernel,
        out_shape=tile((pairs * sources, 1, qw), f32),
        in_specs=[SMEM, VMEM, VMEM, VMEM],
        out_specs=VMEM,
        cost_estimate=cost(1 << 20),
        name="decay",
    )((first_pair // HEADS)[None], low, decay_w, decay_b[None, :])

    tiles = lax.dynamic_slice_in_dim(got, first_head * sources, pairs * sources, 0)
    send = pl.pallas_call(
        functools.partial(read_kernel, qw, vw),
        out_shape=tile((devices, pairs * dv // LANES, LANES), bf16),
        in_specs=[VMEM, VMEM, VMEM, ANY],
        out_specs=VMEM,
        scratch_shapes=[
            pltpu.VMEM((pairs, dk, dv), f32),
            pltpu.SemaphoreType.DMA((pairs, sources)),
        ],
        cost_estimate=cost(pairs * dk * dv * 4),
        name="read",
    )(tiles, decay, head_gain[None, :], head_states)
    got = exchange(send)

    block = pl.BlockSpec((1, qw, dv), lambda p, i: (p, i, 0))
    new_states = pl.pallas_call(
        functools.partial(update_kernel, qw, vw, sources),
        grid=(pairs, sources),
        out_shape=tile(head_states.shape, f32),
        in_specs=[VMEM, VMEM, block],
        out_specs=block,
        cost_estimate=cost(pairs * dk * dv * 8),
        name="update",
    )(tiles, decay, head_states)

    stream, send = pl.pallas_call(
        functools.partial(branch_kernel, chunks),
        out_shape=(tile((tokens, own), bf16), tile((devices, tokens, own), bf16)),
        in_specs=[VMEM, VMEM, ANY],
        out_specs=(VMEM, VMEM),
        scratch_shapes=[
            pltpu.VMEM((width, own), bf16),
            pltpu.SemaphoreType.DMA((1, chunks)),
        ],
        cost_estimate=cost(width * own * 2),
        name="branch",
    )(got, residual, w_output)
    got = exchange(send)

    send = pl.pallas_call(
        functools.partial(expert_kernel, 8),
        out_shape=tile((devices, tokens, own), bf16),
        in_specs=[VMEM] * 3 + [ANY] * 3,
        out_specs=VMEM,
        scratch_shapes=[
            pltpu.VMEM((width, ff), bf16),
            pltpu.VMEM((width, ff), bf16),
            pltpu.VMEM((ff, width), bf16),
            pltpu.SemaphoreType.DMA((2, 8)),
            pltpu.SemaphoreType.DMA((4,)),
        ],
        cost_estimate=cost(width * ff * 6),
        name="expert",
    )(got, second_gain[None, :], share, expert_gate, expert_up, expert_down)
    got = exchange(send)
    layer_out = (stream.astype(f32) + jnp.sum(got.astype(f32), axis=0)).astype(bf16)
    return (layer_out, new_states)


def solution(mesh):
    return jax.shard_map(
        per_device,
        mesh=mesh,
        in_specs=(
            P("grp", "ep"),
            P(("grp", "ep"), None, None),
            P(),
            P(None, "ep"),
            P(None, "ep"),
            P(None, "ep"),
            P(None, "ep"),
            P(),
            P(),
            P(),
            P(),
            P(None, "ep"),
            P(),
            P("grp", None),
            P("grp", None),
            P("grp", None),
            P("ep", None, None),
            P("ep", None, None),
            P("ep", None, None),
        ),
        out_specs=(P("grp", "ep"), P(("grp", "ep"), None, None)),
        check_vma=False,
    )
```

```python
import functools

import jax
import jax.numpy as jnp
from jax import lax
from jax.experimental import pallas as pl
from jax.experimental.pallas import tpu as pltpu
from jax.sharding import PartitionSpec as P

HEADS = 4
GROUPS = 4
LANES = 128
PC, BC, EC, DC = 2, 1, 2, 1
UC, UD = 4, 2

norm_eps = 1e-06
decay_tau = 16.0
f32 = jnp.float32
bf16 = jnp.bfloat16

ANY = pl.BlockSpec(memory_space=pl.ANY)
VMEM = pl.BlockSpec(memory_space=pltpu.VMEM)
SMEM = pl.BlockSpec(memory_space=pltpu.SMEM)


def route_weights(routes, group_logits, expert_logits, per_group):
    group_exp = jnp.exp(group_logits)
    group_prob = group_exp / jnp.sum(group_exp, axis=1, keepdims=True)
    chosen = routes[:, 0] // per_group
    groups_row = jnp.arange(group_logits.shape[1], dtype=jnp.int32)
    picked = jnp.sum(
        group_prob * (chosen[:, None] == groups_row[None, :]).astype(f32), axis=1
    )
    expert_exp = jnp.exp(expert_logits)
    return expert_exp / jnp.sum(expert_exp, axis=1, keepdims=True) * picked[:, None]


def start_chunks(pairs, sems, chunks, both=True):
    started = []
    for c in range(chunks):
        row = []
        for n, (src, dst) in enumerate(pairs):
            size = src.shape[0] // chunks
            rows = pl.ds(c * size, size)
            copy = pltpu.make_async_copy(src.at[rows], dst.at[rows], sems.at[n, c])
            copy.start(priority=(n + c) % 2 if both else 0)
            row.append(copy)
        started.append(row)
    return started


def side_by_side(arrays, buf):
    out, at = [], 0
    for array in arrays:
        wide = array.shape[1]
        out.append((array, buf.at[:, at : at + wide]))
        at += wide
    return out


def start_small(pairs, sems):
    copies = [pltpu.make_async_copy(src, dst, sems.at[n]) for n, (src, dst) in enumerate(pairs)]
    for copy in copies:
        copy.start()
    return copies


def normed_rows(blocks_ref, gain_ref):
    count, _, own = blocks_ref.shape
    total = None
    for j in range(count):
        x = blocks_ref[j].astype(f32)
        total = x * x if total is None else total + x * x
    mean = jnp.sum(total, axis=1, keepdims=True) / (count * own)
    scale = lax.rsqrt(mean + norm_eps)
    out = []
    for j in range(count):
        gain = gain_ref[:, j * own : (j + 1) * own].astype(f32)
        out.append((blocks_ref[j].astype(f32) * scale * gain).astype(bf16))
    return jnp.concatenate(out, axis=1)


def project_kernel(
    chunks,
    blocks,
    gain,
    low_w,
    wq,
    wk,
    wv,
    wg,
    send_ref,
    low_ref,
    *scratch,
):
    *bufs, sems, blocks_ref, gain_ref, low_w_ref, small_sems = scratch
    small = start_small(
        ((blocks, blocks_ref), (gain, gain_ref), (low_w, low_w_ref)), small_sems
    )
    held = [(wq, wk, wv, wg)] if len(bufs) == 1 else [(wq,), (wk,), (wv, wg)]
    places = []
    for arrays, buf in zip(held, bufs):
        places += side_by_side(arrays, buf) if len(arrays) > 1 else [(arrays[0], buf)]
    started = start_chunks(places, sems, chunks)
    for copy in small:
        copy.wait()
    normed = normed_rows(blocks_ref, gain_ref)
    low_ref[...] = lax.dot_general(
        low_w_ref[...], normed, (((1,), (1,)), ((), ())), preferred_element_type=f32
    )
    size = bufs[0].shape[0] // chunks
    sums = [None] * len(bufs)
    for c in range(chunks):
        for copy in started[c]:
            copy.wait()
        part = normed[:, c * size : (c + 1) * size]
        for n, buf in enumerate(bufs):
            one = jnp.dot(part, buf[c * size : (c + 1) * size, :], preferred_element_type=f32)
            sums[n] = one if sums[n] is None else sums[n] + one
    total = jnp.concatenate(sums, axis=1)
    projected = total.astype(bf16).astype(f32)
    rows = projected.shape[1] // LANES
    tokens = projected.shape[0]
    times = send_ref.shape[0] // tokens
    pad = jnp.zeros((send_ref.shape[1] - rows, LANES), f32)
    for s in range(tokens):
        tile = jnp.concatenate(
            [projected[s : s + 1, r * LANES : (r + 1) * LANES] for r in range(rows)] + [pad], axis=0
        )
        for t in range(times):
            send_ref[s * times + t] = tile


def decay_kernel(seq_ref, low_ref, w_ref, bias_ref, _gain, _share, out_ref):
    lane = lax.broadcasted_iota(jnp.int32, low_ref.shape, 1)
    low = jnp.sum(jnp.where(lane == seq_ref[0], low_ref[...], 0.0), axis=1, keepdims=True)
    pre = jnp.sum(w_ref[...].astype(f32) * low, axis=0, keepdims=True) + bias_ref[...]
    log_decay = (jnp.minimum(pre, 0.0) - jnp.log1p(jnp.exp(-jnp.abs(pre)))) / decay_tau
    decay = jnp.exp(log_decay)
    wide = out_ref.shape[2]
    for r in range(out_ref.shape[0]):
        out_ref[r] = decay[:, r * wide : (r + 1) * wide]


def tile_columns(tile, decay, qw):
    if qw < LANES:
        decay = jnp.concatenate([decay, jnp.zeros((1, LANES - qw), f32)], axis=1)
    row = lax.broadcasted_iota(jnp.int32, tile.shape, 0)
    turned = jnp.where(row == tile.shape[0] - 1, decay, tile).T
    last = tile.shape[0] - 1

    def column(at):
        return turned[at % LANES : at % LANES + qw, at // LANES : at // LANES + 1]

    return column(0), column(qw), turned[:qw, last : last + 1]


def wide_row(tiles, at, width):
    pieces = []
    for tile in tiles:
        for lane in range(at, at + width, LANES):
            pieces.append(tile[lane // LANES : lane // LANES + 1, :])
    return jnp.concatenate(pieces, axis=1)


def read_kernel(
    qw, vw, base, got, decay, gain, states, send_ref, buf, sems, tiles_ref, decay_ref, gain_ref, small_sems
):
    pairs, dk, dv = states.shape
    sources = dk // qw
    mine = got.at[pl.ds(base[0], pairs * sources)]
    small = start_small(((mine, tiles_ref), (decay, decay_ref), (gain, gain_ref)), small_sems)
    copies = []
    for p in range(pairs):
        for i in range(sources):
            rows = pl.ds(i * qw, qw)
            copy = pltpu.make_async_copy(
                states.at[p, rows], buf.at[p, rows], sems.at[p, i]
            )
            copy.start(priority=i % 2)
            copies.append(copy)
    for copy in small:
        copy.wait()
    lines = []
    for p in range(pairs):
        tiles = [tiles_ref[p * sources + i] for i in range(sources)]
        value = wide_row(tiles, 2 * qw, vw)
        gate = wide_row(tiles, 2 * qw + vw, vw)
        total = jnp.zeros((8, dv), f32)
        both = jnp.zeros((1, 1), f32)
        for i in range(sources):
            query, key, decay = tile_columns(tiles[i], decay_ref[p * sources + i], qw)
            both = both + jnp.sum(query * key, axis=0, keepdims=True)
            factor = query * decay
            copies[p * sources + i].wait()
            for g in range(qw // 8):
                at = i * qw + g * 8
                total = total + buf[p, at : at + 8, :] * factor[g * 8 : g * 8 + 8]
        read = (jnp.sum(total, axis=0, keepdims=True) + both * value) * dk ** (-0.5)
        mean = jnp.sum(read * read, axis=1, keepdims=True) / dv
        line = read * lax.rsqrt(mean + norm_eps) * gain_ref[...].astype(f32)
        line = line * (gate * (1.0 / (1.0 + jnp.exp(-gate))))
        lines += [line[:, c * LANES : (c + 1) * LANES] for c in range(dv // LANES)]
    mixed = jnp.concatenate(lines, axis=0).astype(bf16)
    for d in range(send_ref.shape[0]):
        send_ref[d] = mixed


def update_kernel(qw, vw, sources, first, base, tiles_ref, decay_ref, state_ref, *rest):
    out_ref, flag_ref = rest[-2:]
    at = first + pl.program_id(0)
    pair = at // sources * sources
    tiles = [tiles_ref[base[0] + pair + n] for n in range(sources)]
    value = wide_row(tiles, 2 * qw, vw)
    _, key, decay = tile_columns(tiles_ref[base[0] + at], decay_ref[at], qw)
    flag_ref[...] = jnp.zeros_like(flag_ref)
    out_ref[0] = state_ref[0] * decay + key * value


def branch_kernel(
    chunks, got, res, w, flag, stream_ref, send_ref, buf, sems, got_ref, res_ref, small_sems
):
    small = start_small(((got, got_ref), (res, res_ref)), small_sems)
    started = start_chunks(((w, buf),), sems, chunks)
    for copy in small:
        copy.wait()
    tokens = res_ref.shape[0]
    parts = got_ref[...].astype(f32).reshape(tokens, -1, LANES)
    parts = jnp.swapaxes(parts, 0, 1)
    size = buf.shape[0] // chunks
    total = None
    for c in range(chunks):
        each = size // LANES
        part = jnp.concatenate([parts[c * each + m] for m in range(each)], axis=1).astype(bf16)
        started[c][0].wait()
        one = jnp.dot(part, buf[c * size : (c + 1) * size, :], preferred_element_type=f32)
        total = one if total is None else total + one
    stream = (res_ref[...].astype(f32) + total.astype(bf16).astype(f32)).astype(bf16)
    stream_ref[...] = stream
    for d in range(send_ref.shape[0]):
        send_ref[d] = stream


def expert_kernel(
    chunks,
    blocks,
    gain,
    share,
    wg,
    wu,
    wd,
    flag,
    send_ref,
    buf,
    bd,
    sems,
    dsems,
    blocks_ref,
    gain_ref,
    share_ref,
    small_sems,
):
    small = start_small(
        ((blocks, blocks_ref), (gain, gain_ref), (share, share_ref)), small_sems
    )
    started = start_chunks(side_by_side((wg.at[0], wu.at[0]), buf), sems, chunks, False)
    own = send_ref.shape[2]
    pieces = DC
    wide = bd.shape[1] // pieces
    downs = []
    for c in range(pieces):
        columns = pl.ds(c * wide, wide)
        copy = pltpu.make_async_copy(wd.at[0, :, columns], bd.at[:, columns], dsems.at[c])
        copy.start()
        downs.append(copy)
    for copy in small:
        copy.wait()
    normed = normed_rows(blocks_ref, gain_ref)
    size = buf.shape[0] // chunks
    total = None
    for c in range(chunks):
        for copy in started[c]:
            copy.wait()
        part = normed[:, c * size : (c + 1) * size]
        one = jnp.dot(part, buf[c * size : (c + 1) * size, :], preferred_element_type=f32)
        total = one if total is None else total + one
    ff = buf.shape[1] // 2
    gate, up = total[:, :ff], total[:, ff:]
    active = gate * (1.0 / (1.0 + jnp.exp(-gate))) * up * share_ref[...]
    active = active.astype(bf16)
    for c in range(pieces):
        downs[c].wait()
        one = jnp.dot(active, bd[:, c * wide : (c + 1) * wide], preferred_element_type=f32)
        one = one.astype(bf16)
        for n in range(wide // own):
            send_ref[c * (wide // own) + n] = one[:, n * own : (n + 1) * own]


def grant(mib):
    return pltpu.CompilerParams(vmem_limit_bytes=mib << 20)


def cost(nbytes):
    return pl.CostEstimate(flops=nbytes, bytes_accessed=nbytes, transcendentals=0)


def exchange(blocks):
    return lax.all_to_all(blocks, "ep", split_axis=0, concat_axis=0, tiled=True)


def per_device(
    residual,
    head_states,
    first_gain,
    w_query,
    w_key,
    w_value,
    w_gate,
    w_low,
    w_decay,
    decay_bias,
    head_gain,
    w_output,
    second_gain,
    routes,
    group_logits,
    expert_logits,
    expert_gate,
    expert_up,
    expert_down,
):
    devices = lax.axis_size("ep")
    me = lax.axis_index("ep")
    tokens, own = residual.shape
    width = own * devices
    pairs, dk, dv = head_states.shape
    qw, vw = w_query.shape[1], w_value.shape[1]
    sources = devices // HEADS
    rank = w_low.shape[1]
    ff = expert_gate.shape[2]
    tile = jax.ShapeDtypeStruct

    arrived = exchange(jnp.broadcast_to(residual[None], (devices, tokens, own)))

    first_pair = me * pairs
    first_head = lax.rem(first_pair, HEADS)
    decay_w = lax.dynamic_slice_in_dim(w_decay, first_head * dk, pairs * dk, 1)
    decay_b = lax.dynamic_slice_in_dim(decay_bias, first_head * dk, pairs * dk, 0)
    weights = route_weights(routes, group_logits, expert_logits, devices // GROUPS)
    share = jnp.sum(weights * (routes == me).astype(f32), axis=1)[:, None]

    gain_row = second_gain[None, :]
    chunks = PC
    columns = [2 * (qw + vw)] if qw % LANES == 0 else [qw, qw, 2 * vw]
    send, low = pl.pallas_call(
        functools.partial(project_kernel, chunks),
        out_shape=(tile((devices, 8, LANES), f32), tile((rank, tokens), f32)),
        in_specs=[ANY] * 7,
        out_specs=(VMEM, VMEM),
        scratch_shapes=[
            *[pltpu.VMEM((width, n), bf16) for n in columns],
            pltpu.SemaphoreType.DMA((4, chunks)),
            pltpu.VMEM((devices, tokens, own), bf16),
            pltpu.VMEM((1, width), bf16),
            pltpu.VMEM((rank, width), bf16),
            pltpu.SemaphoreType.DMA((3,)),
        ],
        compiler_params=grant(60),
        cost_estimate=cost(width * (qw + vw) * 4),
        name="project",
    )(arrived, first_gain[None, :], w_low.T, w_query, w_key, w_value, w_gate)
    got = exchange(send)

    decay = pl.pallas_call(
        decay_kernel,
        out_shape=tile((pairs * sources, 1, qw), f32),
        in_specs=[SMEM, VMEM, VMEM, VMEM, ANY, ANY],
        out_specs=VMEM,
        compiler_params=grant(60),
        cost_estimate=cost(1 << 20),
        name="decay",
    )((first_pair // HEADS)[None], low, decay_w, decay_b[None, :], gain_row, share)

    base = (first_head * sources)[None]
    qkvg = got
    send = pl.pallas_call(
        functools.partial(read_kernel, qw, vw),
        out_shape=tile((devices, pairs * dv // LANES, LANES), bf16),
        in_specs=[SMEM, ANY, ANY, ANY, ANY],
        out_specs=VMEM,
        scratch_shapes=[
            pltpu.VMEM((pairs, dk, dv), f32),
            pltpu.SemaphoreType.DMA((pairs, sources)),
            pltpu.VMEM((pairs * sources, 8, LANES), f32),
            pltpu.VMEM((pairs * sources, 1, qw), f32),
            pltpu.VMEM((1, dv), bf16),
            pltpu.SemaphoreType.DMA((3,)),
        ],
        compiler_params=grant(60),
        cost_estimate=cost(pairs * dk * dv * 4),
        name="read",
    )(base, qkvg, decay, head_gain[None, :], head_states)
    got = exchange(send)

    def update(states, after, first, count):
        block = pl.BlockSpec(
            (1, qw, dv), lambda n: ((first + n) // sources, (first + n) % sources, 0)
        )
        held = [] if states is None else [states]
        return pl.pallas_call(
            functools.partial(update_kernel, qw, vw, sources, first),
            grid=(count,),
            out_shape=(tile(head_states.shape, f32), tile((8, LANES), f32)),
            in_specs=[SMEM, VMEM, VMEM, block, ANY] + [ANY] * len(held),
            out_specs=(block, pl.BlockSpec((8, LANES), lambda n: (0, 0))),
            input_output_aliases={5: 0} if held else {},
            compiler_params=grant(60),
            cost_estimate=cost(count * qw * dv * 8),
            name="update",
        )(base, qkvg, decay, head_states, after, *held)

    blocks = pairs * sources
    new_states, flag = update(None, send, 0, UC * blocks // 8)

    stream, send = pl.pallas_call(
        functools.partial(branch_kernel, BC),
        out_shape=(tile((tokens, own), bf16), tile((devices, tokens, own), bf16)),
        in_specs=[ANY] * 4,
        out_specs=(VMEM, VMEM),
        scratch_shapes=[
            pltpu.VMEM((width, own), bf16),
            pltpu.SemaphoreType.DMA((1, BC)),
            pltpu.VMEM(got.shape, bf16),
            pltpu.VMEM((tokens, own), bf16),
            pltpu.SemaphoreType.DMA((2,)),
        ],
        compiler_params=grant(60),
        cost_estimate=cost(width * own * 2),
        name="branch",
    )(got, residual, w_output, flag)
    got = exchange(send)
    new_states, flag = update(new_states, send, UC * blocks // 8, UD * blocks // 8)

    send = pl.pallas_call(
        functools.partial(expert_kernel, EC),
        out_shape=tile((devices, tokens, own), bf16),
        in_specs=[ANY] * 7,
        out_specs=VMEM,
        scratch_shapes=[
            pltpu.VMEM((width, 2 * ff), bf16),
            pltpu.VMEM((ff, width), bf16),
            pltpu.SemaphoreType.DMA((2, EC)),
            pltpu.SemaphoreType.DMA((DC,)),
            pltpu.VMEM((devices, tokens, own), bf16),
            pltpu.VMEM((1, width), bf16),
            pltpu.VMEM((tokens, 1), f32),
            pltpu.SemaphoreType.DMA((3,)),
        ],
        compiler_params=grant(60),
        cost_estimate=cost(width * ff * 6),
        name="expert",
    )(got, gain_row, share, expert_gate, expert_up, expert_down, flag)
    got = exchange(send)
    if UC + UD < 8:
        done = (UC + UD) * blocks // 8
        new_states, _ = update(new_states, send, done, blocks - done)
    layer_out = (stream.astype(f32) + jnp.sum(got.astype(f32), axis=0)).astype(bf16)
    return (layer_out, new_states)


def solution(mesh):
    return jax.shard_map(
        per_device,
        mesh=mesh,
        in_specs=(
            P("grp", "ep"),
            P(("grp", "ep"), None, None),
            P(),
            P(None, "ep"),
            P(None, "ep"),
            P(None, "ep"),
            P(None, "ep"),
            P(),
            P(),
            P(),
            P(),
            P(None, "ep"),
            P(),
            P("grp", None),
            P("grp", None),
            P("grp", None),
            P("ep", None, None),
            P("ep", None, None),
            P("ep", None, None),
        ),
        out_specs=(P("grp", "ep"), P(("grp", "ep"), None, None)),
        check_vma=False,
    )
```
